256 devices in a mesh: sp: 32 (over z, y), tp: 8 (over x, core).
Axes of the slice: x: 4, y: 4, z: 8, core: 2. Of those that a mesh axis runs over, the one named last changes fastest.
Arguments:
- latent: bfloat16 [16384, 4096], P(('sp', 'tp')), may hold values from -3 to 3
- context: bfloat16 [1024, 4096], P('sp'), may hold values from -6 to 6
- cond: float32 [4096], replicated, may hold values from -6 to 6
- ctx_cond: float32 [4096], replicated, may hold values from -6 to 6
- w_shift: bfloat16 [4096, 4096], P('sp', 'tp'), may hold values from -0.1875 to 0.1875
- w_scale: bfloat16 [4096, 4096], P('sp', 'tp'), may hold values from -0.09375 to 0.15478516
- w_gate: bfloat16 [4096, 4096], P('sp', 'tp'), may hold values from -0.1875 to 0.1875
- w_query: bfloat16 [4096, 2048], P(None, 'tp'), may hold values from -0.09375 to 0.09375
- key_weight: bfloat16 [4096, 1024], P(None, 'tp'), may hold values from -0.09375 to 0.09375
- value_weight: bfloat16 [4096, 1024], P(None, 'tp'), may hold values from -0.09375 to 0.09375
- w_out: bfloat16 [2048, 4096], P('tp'), may hold values from -0.125 to 0.125
- sink: float32 [16], replicated, may hold values from 4 to 8
Outputs:
- mixed: bfloat16 [16384, 4096], P(('sp', 'tp'))
The draws below stay inside these ranges and needn't reach their ends.
All inputs are finite; a program needn't handle non-finite values.
Results may differ from the reference program's by a relative error of at most 0.035.
Values may be sent and summed in bfloat16 or wider, within the bound.
No kernel may reach another device: no remote copies, remote signals or barrier semaphores. Data moves between devices by JAX's collectives and lax.ppermute only.
A program may use at most 64 MiB of HBM per device.

```python
import math
import jax
import jax.numpy as jnp
from jax import lax

MODEL_WIDTH = 4096
HEAD_SIZE = 128
QUERY_HEADS = 16
KEY_VALUE_HEADS = 8
WINDOW_SIDE = 128
GRID_WIDTH = 64
CONTEXT_TOKENS = 1024
LATENT_TOKENS = 16384
N_TP = 8


def draw_w_scale(key, part):
    first, second = jax.random.split(jax.random.fold_in(key, 11))
    spread = 2.0 / math.sqrt(MODEL_WIDTH)
    values = jnp.clip(jax.random.normal(first, (MODEL_WIDTH, MODEL_WIDTH), jnp.float32) * spread, -3.0 * spread, 3.0 * spread)
    return values.astype(jnp.bfloat16)


def level_of(stream_key, dims, cuts, least, largest):
    loudness, own = 1.0, jax.random.fold_in(stream_key, 6)
    for dim, shards_of in cuts:
        draws = jnp.exp(jax.random.uniform(jax.random.fold_in(own, dim), (shards_of,), jnp.float32, least / len(cuts), largest / len(cuts)))
        loudness = loudness * jnp.repeat(draws, dims[dim] // shards_of).reshape([-1 if axis == dim else 1 for axis in range(len(dims))])
    return loudness


def normal_values(stream_key, dims, scale, most, shards=(), kind=jnp.bfloat16):
    level = level_of(stream_key, dims, shards, -0.22, 0.18) if shards else 1.0
    values = jax.random.normal(stream_key, dims, jnp.float32) * scale * level
    return jnp.minimum(jnp.maximum(values, -most), most).astype(kind)


def setup_inputs(seed: int = 0) -> dict:
    splits = jax.random.split(jax.random.key(seed), 13)
    return {
        "latent": normal_values(splits[0], (LATENT_TOKENS, MODEL_WIDTH), 0.5, 3.0, ((0, 256),)),
        "context": normal_values(splits[1], (CONTEXT_TOKENS, MODEL_WIDTH), 1.0, 6.0, ((0, 32),)),
        "cond": normal_values(splits[2], (MODEL_WIDTH,), 1.0, 6.0, (), jnp.float32),
        "ctx_cond": normal_values(splits[3], (MODEL_WIDTH,), 1.0, 6.0, (), jnp.float32),
        "w_shift": normal_values(splits[4], (MODEL_WIDTH, MODEL_WIDTH), (MODEL_WIDTH // 4) ** -0.5, 0.1875, ((0, 32), (1, 8))),
        "w_scale": draw_w_scale(jax.random.fold_in(splits[12], 71), 0),
        "w_gate": normal_values(splits[6], (MODEL_WIDTH, MODEL_WIDTH), (MODEL_WIDTH // 4) ** -0.5, 0.1875, ((0, 32), (1, 8))),
        "w_query": normal_values(splits[7], (MODEL_WIDTH, QUERY_HEADS * HEAD_SIZE), MODEL_WIDTH ** -0.5, 0.09375, ((1, 8),)),
        "key_weight": normal_values(splits[8], (MODEL_WIDTH, KEY_VALUE_HEADS * HEAD_SIZE), MODEL_WIDTH ** -0.5, 0.09375, ((1, 8),)),
        "value_weight": normal_values(splits[9], (MODEL_WIDTH, KEY_VALUE_HEADS * HEAD_SIZE), MODEL_WIDTH ** -0.5, 0.09375, ((1, 8),)),
        "w_out": normal_values(splits[10], (QUERY_HEADS * HEAD_SIZE, MODEL_WIDTH), (QUERY_HEADS * HEAD_SIZE) ** -0.5, 0.125, ((0, 8),)),
        "sink": jnp.clip(jax.random.uniform(splits[11], (QUERY_HEADS,), jnp.float32, 4.0, 8.0), 4.0, 8.0),
    }


EPS = 1e-05
THETA = 10000.0
MASKED = -1e+30

def layer_norm(rows):
    values = rows.astype(jnp.float32)
    mean = lax.optimization_barrier(jnp.mean(values, axis=-1, keepdims=True))
    var = lax.optimization_barrier(jnp.mean(jnp.square(values - mean), axis=-1, keepdims=True))
    return (values - mean) * lax.rsqrt(var + EPS)

def rotate_half(values, token_position, width):
    half = width // 2
    inverse = THETA ** (-jnp.arange(half, dtype=jnp.float32) * 2.0 / width)
    angle = token_position.astype(jnp.float32)[:, None] * inverse[None, :]
    cosine = jnp.cos(angle)[:, None, :]
    sine = jnp.sin(angle)[:, None, :]
    first = values[..., :half]
    second = values[..., half:]
    return jnp.concatenate([first * cosine - second * sine, second * cosine + first * sine], axis=-1)

def axial_rotation(heads, token_position, grid):
    width = heads.shape[-1] // 2
    values = heads.astype(jnp.float32)
    turned = jnp.concatenate([rotate_half(values[..., :width], token_position // grid, width), rotate_half(values[..., width:], token_position % grid, width)], axis=-1)
    return turned.astype(jnp.bfloat16)

def sink_weights(scores, sink_column):
    top = jnp.maximum(lax.optimization_barrier(jnp.max(scores, axis=-1, keepdims=True)), sink_column)
    expo = jnp.exp(scores - top)
    return (expo / (lax.optimization_barrier(jnp.sum(expo, axis=-1, keepdims=True)) + jnp.exp(sink_column - top))).astype(jnp.bfloat16)

def reference(latent, context, cond, ctx_cond, w_shift, w_scale, w_gate, w_query, key_weight, value_weight, w_out, sink):
    act = jax.nn.silu(jnp.stack([cond, ctx_cond])).astype(jnp.bfloat16)
    shift = jnp.dot(act, w_shift, preferred_element_type=jnp.float32)
    scale = jnp.dot(act, w_scale, preferred_element_type=jnp.float32)
    gate = jnp.dot(act[0:1], w_gate, preferred_element_type=jnp.float32)[0]
    latent_mod = (layer_norm(latent) * (1.0 + scale[0]) + shift[0]).astype(jnp.bfloat16)
    ctx_mod = (layer_norm(context) * (1.0 + scale[1]) + shift[1]).astype(jnp.bfloat16)
    query_group = QUERY_HEADS // KEY_VALUE_HEADS
    query = jnp.dot(latent_mod, w_query, preferred_element_type=jnp.float32).astype(jnp.bfloat16)
    key = jnp.dot(latent_mod, key_weight, preferred_element_type=jnp.float32).astype(jnp.bfloat16)
    value_rows = jnp.dot(latent_mod, value_weight, preferred_element_type=jnp.float32).astype(jnp.bfloat16)
    context_key_rows = jnp.dot(ctx_mod, key_weight, preferred_element_type=jnp.float32).astype(jnp.bfloat16)
    context_value_rows = jnp.dot(ctx_mod, value_weight, preferred_element_type=jnp.float32).astype(jnp.bfloat16)
    token_position = jnp.arange(LATENT_TOKENS, dtype=jnp.int32)
    rotated_query = axial_rotation(query.reshape(LATENT_TOKENS, QUERY_HEADS, HEAD_SIZE), token_position, GRID_WIDTH)
    rotated_key = axial_rotation(key.reshape(LATENT_TOKENS, KEY_VALUE_HEADS, HEAD_SIZE), token_position, GRID_WIDTH)
    padded_key = jnp.pad(rotated_key, ((WINDOW_SIDE, WINDOW_SIDE), (0, 0), (0, 0)))
    value_padded_rows = jnp.pad(value_rows.reshape(LATENT_TOKENS, KEY_VALUE_HEADS, HEAD_SIZE), ((WINDOW_SIDE, WINDOW_SIDE), (0, 0), (0, 0)))
    context_key_wide = context_key_rows.reshape(CONTEXT_TOKENS, KEY_VALUE_HEADS, HEAD_SIZE).astype(jnp.float32)
    context_value_wide = context_value_rows.reshape(CONTEXT_TOKENS, KEY_VALUE_HEADS, HEAD_SIZE).astype(jnp.float32)
    sink_column = sink.reshape(KEY_VALUE_HEADS, query_group)[:, :, None, None]
    factor = HEAD_SIZE ** (-0.5)
    block_list = LATENT_TOKENS // WINDOW_SIDE
    query_block_list = rotated_query.reshape(block_list, WINDOW_SIDE, KEY_VALUE_HEADS, query_group, HEAD_SIZE)

    def one_block(item):
        qblk, index = item
        start = (index * WINDOW_SIDE).astype(jnp.int32)
        kblk = lax.dynamic_slice_in_dim(padded_key, start, 3 * WINDOW_SIDE, 0).astype(jnp.float32)
        vblk = lax.dynamic_slice_in_dim(value_padded_rows, start, 3 * WINDOW_SIDE, 0).astype(jnp.float32)
        q32 = qblk.astype(jnp.float32)
        band_scores = jnp.einsum('qhgd,khd->hgqk', q32, kblk) * factor
        qpos = start + jnp.arange(WINDOW_SIDE, dtype=jnp.int32)
        kpos = start - WINDOW_SIDE + jnp.arange(3 * WINDOW_SIDE, dtype=jnp.int32)
        valid = (jnp.abs(kpos[None, :] - qpos[:, None]) <= WINDOW_SIDE) & (kpos[None, :] >= 0) & (kpos[None, :] < LATENT_TOKENS)
        band_scores = jnp.where(valid[None, None], band_scores, MASKED)
        ctx_scores = jnp.einsum('qhgd,khd->hgqk', q32, context_key_wide) * factor
        weights = sink_weights(jnp.concatenate([band_scores, ctx_scores], axis=-1), sink_column).astype(jnp.float32)
        out = jnp.einsum('hgqk,khd->qhgd', weights[..., :3 * WINDOW_SIDE], vblk) + jnp.einsum('hgqk,khd->qhgd', weights[..., 3 * WINDOW_SIDE:], context_value_wide)
        return out.astype(jnp.bfloat16).reshape(WINDOW_SIDE, QUERY_HEADS * HEAD_SIZE)
    attended = lax.map(one_block, (query_block_list, jnp.arange(block_list, dtype=jnp.int32))).reshape(LATENT_TOKENS, QUERY_HEADS * HEAD_SIZE)
    columns = QUERY_HEADS * HEAD_SIZE // N_TP
    projected = jnp.zeros((LATENT_TOKENS, MODEL_WIDTH), jnp.float32)
    for group_index in range(N_TP):
        lower = group_index * columns
        partial_product = jnp.dot(attended[:, lower:lower + columns], w_out[lower:lower + columns], preferred_element_type=jnp.float32).astype(jnp.bfloat16)
        projected = projected + partial_product.astype(jnp.float32)
    return (latent.astype(jnp.float32) + gate[None, :] * projected).astype(jnp.bfloat16)
```

```python
import functools

import jax
import jax.numpy as jnp
from jax import lax
from jax.experimental import pallas as pl
from jax.experimental.pallas import tpu as pltpu
from jax.sharding import PartitionSpec as P

HEAD = 128
SIDE = 128
GRID_WIDTH = 64
EPS = 1e-05
THETA = 10000.0
MASKED = -1e30
LOG2E = 1.4426950408889634

F32 = jnp.float32
BF16 = jnp.bfloat16
ANY = pl.BlockSpec(memory_space=pl.ANY)
VMEM = pl.BlockSpec(memory_space=pltpu.VMEM)
SMEM = pl.BlockSpec(memory_space=pltpu.SMEM)


def cost(flops, moved):
    return pl.CostEstimate(flops=int(flops), bytes_accessed=int(moved), transcendentals=0)


def params(mib=48):
    return pltpu.CompilerParams(vmem_limit_bytes=mib * 1024 * 1024)


def dot(a, b):
    return jnp.dot(a, b, preferred_element_type=F32)


def dot_nt(a, b):
    return lax.dot_general(a, b, (((1,), (1,)), ((), ())), preferred_element_type=F32)


def modulation_part(index, cond, ctx_cond, w_shift, w_scale, w_gate, count):
    rows, cols = w_shift.shape

    def kernel(index_ref, cond_ref, ctx_ref, shift_ref, scale_ref, gate_ref, out_ref):
        own = pl.ds(index_ref[0], 1)
        first = cond_ref[own, :]
        second = ctx_ref[own, :]
        line = lax.broadcasted_iota(jnp.int32, (8, rows), 0)
        both = jnp.where(line == 0, first, jnp.where(line == 1, second, 0.0))
        act = (both / (1.0 + jnp.exp(-both))).astype(BF16)
        shift = dot(act, shift_ref[...])
        scale = dot(act, scale_ref[...])
        gate = dot(act, gate_ref[...])
        part = jnp.concatenate([shift[0:2], scale[0:2], gate[0:1], jnp.zeros((3, cols), F32)], axis=0)
        part = part.astype(BF16)
        for k in range(count):
            out_ref[k] = part

    return pl.pallas_call(
        kernel,
        out_shape=jax.ShapeDtypeStruct((count, 8, cols), BF16),
        in_specs=[SMEM] + [VMEM] * 5,
        out_specs=VMEM,
        compiler_params=params(),
        cost_estimate=cost(3 * 2 * 8 * rows * cols * 20, 3 * rows * cols * 2),
        name="modulation_part",
    )(index, cond.reshape(-1, rows), ctx_cond.reshape(-1, rows), w_shift, w_scale, w_gate)


def modulation_sum(parts, copies):
    count, rows, cols = parts.shape

    def kernel(parts_ref, out_ref):
        total = jnp.sum(parts_ref[...].astype(F32), axis=0)
        for k in range(copies):
            out_ref[k] = total

    return pl.pallas_call(
        kernel,
        out_shape=jax.ShapeDtypeStruct((copies, rows, cols), F32),
        in_specs=[VMEM],
        out_specs=VMEM,
        compiler_params=params(),
        cost_estimate=cost(1e7, count * rows * cols * 2),
        name="modulation_sum",
    )(parts)


def row_of(mod_ref, line):
    return jnp.concatenate([mod_ref[t, line : line + 1, :] for t in range(mod_ref.shape[0])], axis=1)


def normed(x, scale, shift):
    mean = jnp.mean(x, axis=-1, keepdims=True)
    centred = x - mean
    var = jnp.mean(centred * centred, axis=-1, keepdims=True)
    return (centred * lax.rsqrt(var + EPS) * (1.0 + scale) + shift).astype(BF16)


def context_pairs(context, mod, key_weight, value_weight, count):
    tokens, width = context.shape
    cols = key_weight.shape[1]

    def kernel(ctx_ref, mod_ref, key_ref, value_ref, out_ref):
        rows = normed(ctx_ref[...].astype(F32), row_of(mod_ref, 3), row_of(mod_ref, 1))
        pair = jnp.concatenate([dot(rows, key_ref[...]), dot(rows, value_ref[...])], axis=1).astype(BF16)
        for k in range(count):
            out_ref[k] = pair

    return pl.pallas_call(
        kernel,
        out_shape=jax.ShapeDtypeStruct((count, tokens, 2 * cols), BF16),
        in_specs=[VMEM] * 4,
        out_specs=VMEM,
        compiler_params=params(),
        cost_estimate=cost(2e9, 3e6),
        name="context_pairs",
    )(context, mod, key_weight, value_weight)


def rotary_tables(position):
    lane = jnp.arange(HEAD, dtype=jnp.int32)
    width = HEAD // 2
    inverse = THETA ** (-(lane % (width // 2)).astype(F32) * 2.0 / width)
    row = (position // GRID_WIDTH).astype(F32)
    col = (position % GRID_WIDTH).astype(F32)
    angle = jnp.where(lane[None, :] < width, row[:, None], col[:, None]) * inverse[None, :]
    sign = jnp.where(lane % width < width // 2, -1.0, 1.0).astype(F32)
    return jnp.cos(angle), jnp.sin(angle) * sign[None, :]


def turned(x, cosine, sine):
    x = x.astype(BF16).astype(F32)
    quarter = HEAD // 4
    lane = lax.broadcasted_iota(jnp.int32, x.shape, 1)
    other = jnp.where(
        lane % (2 * quarter) < quarter,
        pltpu.roll(x, HEAD - quarter, 1),
        pltpu.roll(x, quarter, 1),
    )
    return (x * cosine + other * sine).astype(BF16)


def projections(place, pieces, mod, w_query, key_weight, value_weight, cosine, sine):
    width = w_query.shape[0]
    q_cols, kv_cols = w_query.shape[1], key_weight.shape[1]
    flat, where = [], []
    chips = len(pieces)
    for r, sides in enumerate(pieces):
        for side, parts in enumerate(sides):
            at = 0
            for part in parts:
                flat.append(part)
                where.append((r, side, at, part.shape[0]))
                at += part.shape[0]
            half = at
    block = 2 * half
    tokens = chips * block
    n = len(flat)

    def kernel(place_ref, *refs):
        part_refs = refs[:n]
        mod_ref, q_w, k_w, v_w, cos_ref, sin_ref = refs[n : n + 6]
        q_out, kv_out, head_out, tail_out = refs[n + 6 : n + 10]
        x_ref, wq_ref, wk_ref, wv_ref, part_sems, weight_sems = refs[n + 10 :]
        chip, core = place_ref[1], place_ref[2]
        weights = [
            pltpu.make_async_copy(source, target, weight_sems.at[k])
            for k, (source, target) in enumerate(((k_w, wk_ref), (v_w, wv_ref), (q_w, wq_ref)))
        ]
        copies = []
        for k, (r, side, at, length) in enumerate(where):
            to = core if side == 0 else 1 - core
            copies.append(
                pltpu.make_async_copy(part_refs[k], x_ref.at[r, to, pl.ds(at, length)], part_sems.at[k])
            )
        for k, copy in enumerate(copies):
            if where[k][0] == 0:
                copy.start()
        for copy in weights:
            copy.start()
        for k, copy in enumerate(copies):
            if where[k][0] != 0:
                copy.start()
        scale, shift = row_of(mod_ref, 2), row_of(mod_ref, 0)
        for r in range(chips):
            for k, copy in enumerate(copies):
                if where[k][0] == r:
                    copy.wait()
            rows = normed(x_ref[r].reshape(block, width).astype(F32), scale, shift)
            if r == 0:
                for copy in weights:
                    copy.wait()
            place_of = lax.rem(chip + r, chips)
            at = pl.ds(pl.multiple_of(place_of * block, block), block)
            cos, sin = cos_ref[at, :], sin_ref[at, :]
            key = turned(dot(rows, wk_ref[...]), cos, sin)
            value = dot(rows, wv_ref[...]).astype(BF16)
            pair = jnp.concatenate([key, value], axis=1)
            kv_out[at, :] = pair

            @pl.when(place_of == 0)
            def _():
                head_out[...] = pair

            @pl.when(place_of == chips - 1)
            def _():
                tail_out[...] = pair

            query = dot(rows, wq_ref[...])
            for h in range(q_cols // HEAD):
                q_out[at, h * HEAD : (h + 1) * HEAD] = turned(query[:, h * HEAD : (h + 1) * HEAD], cos, sin)

    return pl.pallas_call(
        kernel,
        out_shape=(
            jax.ShapeDtypeStruct((tokens, q_cols), BF16),
            jax.ShapeDtypeStruct((tokens, 2 * kv_cols), BF16),
            jax.ShapeDtypeStruct((block, 2 * kv_cols), BF16),
            jax.ShapeDtypeStruct((block, 2 * kv_cols), BF16),
        ),
        in_specs=[SMEM] + [ANY] * n + [VMEM] + [ANY] * 3 + [VMEM] * 2,
        out_specs=(VMEM,) * 4,
        scratch_shapes=[
            pltpu.VMEM((chips, 2, half, width), BF16),
            pltpu.VMEM((width, q_cols), BF16),
            pltpu.VMEM((width, kv_cols), BF16),
            pltpu.VMEM((width, kv_cols), BF16),
            pltpu.SemaphoreType.DMA((n,)),
            pltpu.SemaphoreType.DMA((3,)),
        ],
        compiler_params=params(),
        cost_estimate=cost(8e9, 8e6),
        name="projections",
    )(place, *flat, mod, w_query, key_weight, value_weight, cosine, sine)


def attention(place, order, query, pairs, before, after, ctx_pairs, sink, chips, total):
    tokens, q_cols = query.shape
    block = tokens // chips
    half = block // 2
    heads = q_cols // HEAD
    kv_cols = pairs.shape[1] // 2
    ctx_tokens = ctx_pairs.shape[0]
    n = len(order)
    factor = LOG2E * HEAD**-0.5

    def kernel(place_ref, sink_ref, q_ref, kv_ref, before_ref, after_ref, ctx_ref, mine_out, other_out, ext_ref, sems):
        sp, chip, core = place_ref[0], place_ref[1], place_ref[2]
        copies = [
            pltpu.make_async_copy(before_ref, ext_ref.at[pl.ds(0, SIDE)], sems.at[0]),
            pltpu.make_async_copy(kv_ref, ext_ref.at[pl.ds(SIDE, tokens)], sems.at[1]),
            pltpu.make_async_copy(after_ref, ext_ref.at[pl.ds(SIDE + tokens, SIDE)], sems.at[2]),
        ]
        for copy in copies:
            copy.start()
        for copy in copies:
            copy.wait()
        ctx_key = ctx_ref[:, :kv_cols]
        ctx_value = ctx_ref[:, kv_cols:]
        rows = heads * block
        i = lax.rem(lax.broadcasted_iota(jnp.int32, (rows, 3 * SIDE), 0), block)
        j = lax.broadcasted_iota(jnp.int32, (rows, 3 * SIDE), 1)
        line = lax.broadcasted_iota(jnp.int32, (rows, 1), 0)
        sink_column = jnp.zeros((rows, 1), F32)
        for h in range(heads):
            sink_column = jnp.where(line // block == h, sink_ref[place_ref[3] + h] * LOG2E, sink_column)
        for k, r in enumerate(order):
            place_of = lax.rem(chip + r, chips)
            at = pl.multiple_of(place_of * block, block)
            q = q_ref[pl.ds(at, block), :]
            q = jnp.concatenate([q[:, h * HEAD : (h + 1) * HEAD] for h in range(heads)], axis=0)
            window = pl.ds(at, 3 * SIDE)
            position = sp * tokens + at - SIDE + j
            valid = (j >= i) & (j <= i + 2 * SIDE) & (position >= 0) & (position < total)
            near = jnp.where(valid, dot_nt(q, ext_ref[window, :kv_cols]) * factor, MASKED)
            far = dot_nt(q, ctx_key) * factor
            top = jnp.maximum(
                jnp.maximum(jnp.max(near, axis=-1, keepdims=True), jnp.max(far, axis=-1, keepdims=True)),
                sink_column,
            )
            near = jnp.exp2(near - top)
            far = jnp.exp2(far - top)
            whole = (
                jnp.sum(near, axis=-1, keepdims=True)
                + jnp.sum(far, axis=-1, keepdims=True)
                + jnp.exp2(sink_column - top)
            )
            out = dot(near.astype(BF16), ext_ref[window, kv_cols:]) + dot(far.astype(BF16), ctx_value)
            out = (out / whole).astype(BF16)
            out = jnp.concatenate([out[h * block : (h + 1) * block] for h in range(heads)], axis=1)
            south, north = out[:half], out[half:]
            mine_out[k * half : (k + 1) * half] = jnp.where(core == 0, south, north)
            other_out[k * half : (k + 1) * half] = jnp.where(core == 0, north, south)

    return pl.pallas_call(
        kernel,
        out_shape=(jax.ShapeDtypeStruct((n * half, q_cols), BF16),) * 2,
        in_specs=[SMEM, SMEM, VMEM, ANY, ANY, ANY, VMEM],
        out_specs=(VMEM,) * 2,
        scratch_shapes=[pltpu.VMEM((tokens + 2 * SIDE, 2 * kv_cols), BF16), pltpu.SemaphoreType.DMA((3,))],
        compiler_params=params(),
        cost_estimate=cost(n * 1.5e9, 2e6),
        name=f"attention_{n}",
    )(place, sink, query, pairs, before, after, ctx_pairs)


def out_projection(mine, other, w_mine, w_other, cuts, types):
    rows, depth = mine.shape
    width = w_mine.shape[1]
    tile = 512

    def kernel(mine_ref, other_ref, w_mine_ref, w_other_ref, *outs):
        total = dot(mine_ref[...], w_mine_ref[...]) + dot(other_ref[...], w_other_ref[...])
        at = 0
        for out, length in zip(outs, cuts):
            out[...] = total[at : at + length].astype(out.dtype)
            at += length

    return pl.pallas_call(
        kernel,
        grid=(width // tile,),
        out_shape=tuple(jax.ShapeDtypeStruct((c, width), t) for c, t in zip(cuts, types)),
        in_specs=[pl.BlockSpec((rows, depth), lambda k: (0, 0))] * 2
        + [pl.BlockSpec((depth, tile), lambda k: (0, k))] * 2,
        out_specs=tuple(pl.BlockSpec((c, tile), lambda k: (0, k)) for c in cuts),
        compiler_params=params(),
        cost_estimate=cost(2 * rows * 2 * depth * width * 4, 4e6),
        name=f"out_projection_{rows}",
    )(mine, other, w_mine, w_other)


def shards(
    latent,
    context,
    cond,
    ctx_cond,
    w_shift,
    w_scale,
    w_gate,
    w_query,
    key_weight,
    value_weight,
    w_out,
    sink,
):
    sp_count = lax.axis_size("sp")
    tp_count = lax.axis_size("tp")
    sp = lax.axis_index("sp")
    tp = lax.axis_index("tp")
    chips = tp_count // 2
    q_heads = w_query.shape[1] // HEAD
    place = jnp.stack([sp, tp // 2, tp % 2, tp * q_heads]).astype(jnp.int32)
    to_right = [(i, (i + 2) % tp_count) for i in range(tp_count)]
    to_left = [(i, (i - 2) % tp_count) for i in range(tp_count)]
    swap = [(i, i ^ 1) for i in range(tp_count)]

    def right(v):
        return lax.ppermute(v, "tp", to_right)

    def left(v):
        return lax.ppermute(v, "tp", to_left)

    def across(v):
        return lax.ppermute(v, "tp", swap)

    half = latent.shape[0]
    cut = half // 2
    from_left = right(latent)
    from_right = left(latent)
    own_other = across(latent)

    parts = modulation_part(place, cond, ctx_cond, w_shift, w_scale, w_gate, sp_count)
    parts = lax.all_to_all(parts, "sp", 0, 0, tiled=True)
    w_out_other = across(w_out)

    far_a = right(from_left[:cut])
    far_b = left(from_right[cut:])
    left_other = across(from_left)
    right_other = across(from_right)

    mod = lax.all_to_all(modulation_sum(parts, tp_count), "tp", 0, 0, tiled=True)
    far_a_other = across(far_a)
    far_b_other = across(far_b)

    ctx_pairs = context_pairs(context, mod, key_weight, value_weight, sp_count)
    ctx_pairs = lax.all_to_all(ctx_pairs, "sp", 0, 0, tiled=True)
    ctx_pairs = ctx_pairs.reshape(-1, ctx_pairs.shape[-1])

    tokens = half * tp_count
    position = sp * tokens + jnp.arange(tokens, dtype=jnp.int32)
    cosine, sine = rotary_tables(position)
    pieces = [
        ((latent,), (own_other,)),
        ((from_right,), (right_other,)),
        ((far_a, far_b), (far_a_other, far_b_other)),
        ((from_left,), (left_other,)),
    ]
    query, pairs, first, last = projections(
        place, pieces, mod, w_query, key_weight, value_weight, cosine, sine
    )
    before = lax.ppermute(last, "sp", [(i, i + 1) for i in range(sp_count - 1)])
    after = lax.ppermute(first, "sp", [(i + 1, i) for i in range(sp_count - 1)])

    attend = functools.partial(
        attention,
        query=query,
        pairs=pairs,
        before=before,
        after=after,
        ctx_pairs=ctx_pairs,
        sink=sink,
        chips=chips,
        total=tokens * sp_count,
    )
    far_mine, far_away = attend(place, (2,))
    far_got = across(far_away)
    rest_mine, rest_away = attend(place, (1, 3, 0))
    rest_got = across(rest_away)
    send_a, send_b = out_projection(far_mine, far_got, w_out, w_out_other, (cut, cut), (BF16,) * 2)
    hop_a = right(send_a)
    hop_b = left(send_b)
    right_a, right_b, left_a, left_b, own = out_projection(
        rest_mine, rest_got, w_out, w_out_other, (cut,) * 4 + (half,), (BF16,) * 4 + (F32,)
    )
    got_left_b = right(right_b)
    got_right_a = left(left_a)
    got_left_a = right((right_a.astype(F32) + hop_a.astype(F32)).astype(BF16))
    got_right_b = left((left_b.astype(F32) + hop_b.astype(F32)).astype(BF16))
    gate = mod[:, 4, :].reshape(1, -1)
    projected = own + jnp.concatenate(
        [
            got_left_a.astype(F32) + got_right_a.astype(F32),
            got_left_b.astype(F32) + got_right_b.astype(F32),
        ],
        axis=0,
    )
    return (latent.astype(F32) + gate * projected).astype(BF16)


def solution(mesh):
    in_specs = (
        P(("sp", "tp"), None),
        P("sp", None),
        P(),
        P(),
        P("sp", "tp"),
        P("sp", "tp"),
        P("sp", "tp"),
        P(None, "tp"),
        P(None, "tp"),
        P(None, "tp"),
        P("tp", None),
        P(),
    )
    out_specs = P(("sp", "tp"), None)
    return jax.shard_map(shards, mesh=mesh, in_specs=in_specs, out_specs=out_specs, check_vma=False)
```
